1024 devices in a mesh: sp: 128 (over z, y), tp: 8 (over x, core).
Axes of the slice: x: 4, y: 4, z: 32, core: 2. Of those that a mesh axis runs over, the one named last changes fastest.
Arguments:
- tokens: bfloat16 [2, 8192, 4096], P(None, 'sp'), may hold values from -28 to 28
- w_forget: bfloat16 [4096, 2048], P(None, 'tp'), may hold values from -0.09375 to 0.09375
- w_value: bfloat16 [4096, 2048], P(None, 'tp'), may hold values from -0.375 to 0.375
- floor_logit: float32 [2048], P('tp'), may hold values from 0.5 to 11.5
- norm_gain: float32 [128], replicated, may hold values from 0.1 to 1.9
- query_new: bfloat16 [2, 2048], P(None, 'tp'), may hold values from -6 to 6
- gate_new: bfloat16 [2, 2048], P(None, 'tp'), may hold values from -6 to 6
- w_out: bfloat16 [2048, 4096], P('tp'), may hold values from -0.125 to 0.125
Outputs:
- state_cache: bfloat16 [2, 16, 128, 128], P(None, 'tp', 'sp')
- decode_out: bfloat16 [2, 4096], P(None, 'tp')
The draws below stay inside these ranges and needn't reach their ends.
All inputs are finite; a program needn't handle non-finite values.
Results may differ from the reference program's by a relative error of at most 0.014.
Values may be sent and summed in bfloat16 or wider, within the bound.
A program may use at most 64 MiB of HBM per device.

```python
import jax
import jax.numpy as jnp
from jax import lax

D = 4096
HEADS = 16
DK = 128
DV = 128
SEQS = 2
SPAN = 64
LENGTH = 8192
N_TP = 8


def draw_tokens(key, part):
    base_key, fine_key, coarse_key, lean_key, shift_key = jax.random.split(jax.random.fold_in(key, 11), 5)
    base = jnp.clip(jax.random.normal(base_key, (SEQS, LENGTH, D), jnp.float32), -4.0, 4.0)
    fine = jnp.exp(jax.random.uniform(fine_key, (SEQS, LENGTH // 8, 1, 1), jnp.float32, jnp.log(0.35), jnp.log(2.8)))
    fine = jnp.broadcast_to(fine, (SEQS, LENGTH // 8, 8, 1)).reshape(SEQS, LENGTH, 1)
    coarse = jnp.exp(jax.random.uniform(coarse_key, (SEQS, 16, 1, 1), jnp.float32, jnp.log(0.4), jnp.log(2.5)))
    coarse = jnp.broadcast_to(coarse, (SEQS, 16, LENGTH // 16, 1)).reshape(SEQS, LENGTH, 1)
    lean = 2.0 * jax.random.normal(lean_key, (1, 1, D), jnp.float32)
    shift = jax.random.uniform(shift_key, (SEQS, LENGTH // SPAN, 1, 1), jnp.float32, -2.5, 2.5)
    shift = jnp.broadcast_to(shift, (SEQS, LENGTH // SPAN, SPAN, 1)).reshape(SEQS, LENGTH, 1)
    mixed = base * fine * coarse + shift * lean
    return jnp.clip(mixed, -28.0, 28.0).astype(jnp.bfloat16)


def draw_floor_logit(key, part):
    kind_key, pick_key, rate_key, jitter_key = jax.random.split(jax.random.fold_in(key, 23), 4)
    kinds = jax.random.randint(kind_key, (HEADS, 1), 0, 3)
    forced = jax.random.randint(pick_key, (), 0, HEADS)
    kinds = jnp.where(jnp.arange(HEADS)[:, None] == forced, 1, kinds)
    low = jnp.where(kinds == 0, jnp.log(0.025), jnp.where(kinds == 1, jnp.log(0.6 / SPAN), jnp.log(3.0 / LENGTH)))
    high = jnp.where(kinds == 0, jnp.log(0.06), jnp.where(kinds == 1, jnp.log(1.6 / SPAN), jnp.log(4.5 / LENGTH)))
    pick = jax.random.uniform(rate_key, (HEADS, 1), jnp.float32)
    jitter = jax.random.uniform(jitter_key, (HEADS, DK), jnp.float32, jnp.log(0.8), jnp.log(1.25))
    leak = jnp.exp(low + pick * (high - low) + jitter)
    logit = jnp.log(1.0 - leak) - jnp.log(leak)
    return logit.astype(jnp.float32).reshape(HEADS * DK)


def levels(key, extent, cuts, low, largest):
    factor_of = 1.0
    for position, blocks in cuts:
        draws = jax.random.uniform(jax.random.fold_in(jax.random.fold_in(key, 6), position), (blocks,), jnp.float32, low / len(cuts), largest / len(cuts))
        factor_of = factor_of * jnp.repeat(jnp.exp(draws), extent[position] // blocks).reshape((-1,) + (1,) * (len(extent) - 1 - position))
    return factor_of


def noise(own_key, extent, deviation, limit, pieces=(), dtype=jnp.bfloat16):
    array = jax.random.normal(own_key, extent, jnp.float32) * deviation
    if len(pieces) > 0:
        array = levels(own_key, extent, pieces, -0.22, 0.18) * array
    return jnp.clip(array, min=-limit, max=limit).astype(dtype)


def setup_inputs(seed: int = 0) -> dict:
    seeds = jax.random.split(jax.random.key(seed), 9)
    return {
        "tokens": draw_tokens(jax.random.fold_in(seeds[8], 71), 0),
        "w_forget": noise(seeds[1], (D, HEADS * DK), D ** -0.5, 0.09375, ((1, 8),)),
        "w_value": noise(seeds[2], (D, HEADS * DV), (D // 16) ** -0.5, 0.375, ((1, 8),)),
        "floor_logit": draw_floor_logit(jax.random.fold_in(seeds[8], 71), 0),
        "norm_gain": jnp.clip(1.0 + 0.18 * jax.random.normal(seeds[4], (DV,), jnp.float32), 0.1, 1.9),
        "query_new": noise(seeds[5], (SEQS, HEADS * DK), 1.0, 6.0, ((1, 8),)),
        "gate_new": noise(seeds[6], (SEQS, HEADS * DV), 1.0, 6.0, ((1, 8),)),
        "w_out": noise(seeds[7], (HEADS * DV, D), (HEADS * DV) ** -0.5, 0.125, ((0, 8),)),
    }


epsilon = 1e-06

def forget_terms(forget_pre, floor_heads):
    forget_f32 = forget_pre.astype(jnp.float32)
    log_keep = jnp.logaddexp(jax.nn.log_sigmoid(floor_heads), jax.nn.log_sigmoid(-floor_heads) + jax.nn.log_sigmoid(forget_f32))
    key_gate = jax.nn.sigmoid(-floor_heads) * jax.nn.sigmoid(-forget_f32)
    return (log_keep, key_gate)

def span_state(block_tokens, w_forget, w_value, floor_heads):
    num_seqs, span_len, model_width = block_tokens.shape
    flat = block_tokens.reshape(num_seqs * span_len, model_width)
    forget_pre = jnp.dot(flat, w_forget, preferred_element_type=jnp.float32).astype(jnp.bfloat16)
    values = jnp.dot(flat, w_value, preferred_element_type=jnp.float32).astype(jnp.bfloat16)
    forget_pre = forget_pre.reshape(num_seqs, span_len, floor_heads.shape[0], floor_heads.shape[1])
    values = values.reshape(num_seqs, span_len, floor_heads.shape[0], -1)
    log_keep, key_gate = forget_terms(forget_pre, floor_heads)
    running = jnp.cumsum(log_keep, axis=1)
    block_total = running[:, -1]
    weighted = key_gate * jnp.exp(block_total[:, None] - running)
    own_state = jnp.einsum('nshk,nshv->nhkv', weighted, values.astype(jnp.float32), precision=lax.Precision.HIGHEST)
    return (block_total, own_state)

def gated_read(read_raw, norm_gain, gate_new):
    scale = lax.rsqrt(lax.optimization_barrier(jnp.mean(read_raw * read_raw, axis=-1, keepdims=True)) + epsilon)
    normed = read_raw * scale * norm_gain
    normed = normed.reshape(normed.shape[0], -1)
    return (normed * jax.nn.silu(gate_new.astype(jnp.float32))).astype(jnp.bfloat16)

def reference(tokens, w_forget, w_value, floor_logit, norm_gain, query_new, gate_new, w_out):
    floor_heads = floor_logit.reshape(HEADS, DK)
    blocks = jnp.moveaxis(tokens.reshape(SEQS, LENGTH // SPAN, SPAN, D), 1, 0)

    def advance(carried, block_tokens):
        block_total, own_state = span_state(block_tokens, w_forget, w_value, floor_heads)
        return (jnp.exp(block_total)[..., None] * carried + own_state, None)
    start_state = jnp.zeros((SEQS, HEADS, DK, DV), jnp.float32)
    final_state, _ = lax.scan(advance, start_state, blocks)
    state_cache = final_state.astype(jnp.bfloat16)
    query = jax.nn.silu(query_new.astype(jnp.float32)).reshape(SEQS, HEADS, DK)
    read_raw = jnp.einsum('nhk,nhkv->nhv', query, final_state, precision=lax.Precision.HIGHEST)
    read = gated_read(read_raw, norm_gain, gate_new)
    groups = read.reshape(SEQS, N_TP, -1).astype(jnp.float32)
    weight_groups = w_out.reshape(N_TP, -1, D).astype(jnp.float32)
    partial_value = jnp.einsum('ntg,tgd->tnd', groups, weight_groups).astype(jnp.bfloat16)
    partial_value = lax.optimization_barrier(partial_value)
    decode_out = lax.optimization_barrier(jnp.sum(partial_value.astype(jnp.float32), axis=0)).astype(jnp.bfloat16)
    return (state_cache, decode_out)
```

```python
import functools

import jax
import jax.numpy as jnp
from jax import lax
from jax.experimental import pallas as pl
from jax.experimental.pallas import tpu as pltpu
from jax.sharding import PartitionSpec as P

MESH = pl.DeviceIdType.MESH
F32 = jnp.float32
BF16 = jnp.bfloat16
EPSILON = 1e-06

DK = 128
PLANE = 16
GROUPS = 8
ROWS = 32
N_TP = 8
CHUNKS = 4
SENDS = (4, 3, 5, 2, 6, 1, 7)


def kernel(
    tok, w_forget, w_value, floor, gain, query, gate, w_out,
    state_out, decode_out,
    tok_v, wf_v, wv_v, wo_v, floor_v, gain_v, query_v, gate_v,
    send1, total1, recv1, rtotal1,
    send3, total3, recv3, rtotal3,
    part4, recv4, row4, rrow4, send5, recv5,
    in_sem, small_sem, wo_sem,
    s1, r1, st1, rt1, s3, r3, st3, rt3, s4, r4, sr4, rr4, s5, r5,
):
    sp, tp = lax.axis_index("sp"), lax.axis_index("tp")
    group, me = sp // PLANE, sp % PLANE
    slice_m, pair = me // 4, me % 4
    depth = tok.shape[1] // CHUNKS

    loads = []
    for c in range(CHUNKS):
        ks = pl.ds(c * depth, depth)
        loads.append([
            pltpu.make_async_copy(tok.at[:, ks], tok_v.at[:, ks], in_sem.at[3 * c]),
            pltpu.make_async_copy(w_forget.at[ks], wf_v.at[ks], in_sem.at[3 * c + 1]),
            pltpu.make_async_copy(w_value.at[ks], wv_v.at[ks], in_sem.at[3 * c + 2]),
        ])
    smalls = [
        pltpu.make_async_copy(src, dst, small_sem.at[i])
        for i, (src, dst) in enumerate(((floor, floor_v), (gain, gain_v), (query, query_v), (gate, gate_v)))
    ]
    load_out = pltpu.make_async_copy(w_out, wo_v, wo_sem)
    for copy in loads[0]:
        copy.start()
    for copy in smalls:
        copy.start()
    for chunk in loads[1:]:
        for copy in chunk:
            copy.start()
    load_out.start()

    barrier = pltpu.get_barrier_semaphore()

    def in_plane(j):
        other = (me + j) % PLANE
        return other, (group * PLANE + other, tp)

    def in_line(j):
        other = (group + j) % GROUPS
        return other, (other * PLANE + me, tp)

    def in_tp(j):
        other = (tp + j) % N_TP
        return other, (sp, other)

    partners = [in_line(j)[1] for j in SENDS]
    partners += [in_plane(j)[1] for j in range(1, PLANE)]
    partners += [in_tp(j)[1] for j in range(1, N_TP)]
    for device in partners:
        pl.semaphore_signal(barrier, inc=1, device_id=device, device_id_type=MESH)

    def remote(src, dst, send_sem, recv_sem, device):
        return pltpu.make_async_remote_copy(
            src_ref=src, dst_ref=dst, send_sem=send_sem, recv_sem=recv_sem, device_id=device, device_id_type=MESH
        )

    forget_acc = jnp.zeros((2 * 64, 2 * DK), F32)
    value_acc = jnp.zeros((2 * 64, 2 * DK), F32)
    for c in range(CHUNKS):
        for copy in loads[c]:
            copy.wait()
        ks = pl.ds(c * depth, depth)
        block = tok_v[:, ks]
        forget_acc += jnp.dot(block, wf_v[ks, :], preferred_element_type=F32)
        value_acc += jnp.dot(block, wv_v[ks, :], preferred_element_type=F32)
    for copy in smalls:
        copy.wait()
    forget_pre = forget_acc.astype(BF16).astype(F32)
    values = value_acc.astype(BF16)

    def sigmoid(x):
        return 1.0 / (1.0 + jnp.exp(-x))

    key_gate = sigmoid(-floor_v[...]) * sigmoid(-forget_pre)
    log_keep = jnp.log1p(-key_gate)
    for n in range(2):
        total = jnp.sum(log_keep[64 * n : 64 * n + 64], axis=0, keepdims=True)
        for h in range(2):
            total1[2 * n + h] = total[:, DK * h : DK * (h + 1)]

    pos = lax.broadcasted_iota(jnp.int32, (128, 128), 0)
    later = lax.broadcasted_iota(jnp.int32, (128, 128), 1)
    after = jnp.where((later > pos) & (later // 64 == pos // 64), 1.0, 0.0).astype(F32)
    decay = jnp.dot(after, log_keep, preferred_element_type=F32, precision=lax.Precision.HIGHEST)
    weighted = (key_gate * jnp.exp(decay)).astype(BF16)

    key_of = 16 * ((pos % 32) // 4) + 4 * (pos // 32) + pos % 4
    permute = jnp.where(later == key_of, 1.0, 0.0).astype(BF16)
    first = lax.broadcasted_iota(jnp.int32, (128, DK), 0) < 64
    for h in range(2):
        cols = slice(DK * h, DK * (h + 1))
        keys = lax.dot_general(
            permute, weighted[:, cols], (((1,), (1,)), ((), ())), preferred_element_type=F32
        ).astype(BF16)
        v = values[:, cols].astype(F32)
        both = jnp.concatenate([jnp.where(first, v, 0.0), jnp.where(first, 0.0, v)], axis=1).astype(BF16)
        own = jnp.dot(keys, both, preferred_element_type=F32).astype(BF16)
        for n in range(2):
            send1[2 * n + h] = own[:, DK * n : DK * (n + 1)]

    pl.semaphore_wait(barrier, len(partners))

    def rows_for(other):
        return send1.at[other % 4, pl.ds(pl.multiple_of(ROWS * (other // 4), ROWS), ROWS)]

    sends = []
    for j in range(1, PLANE):
        other, device = in_plane(j)
        sends.append(remote(total1.at[other % 4], rtotal1.at[me], st1.at[j], rt1.at[me], device))
        sends[-1].start()
        sends.append(remote(rows_for(other), recv1.at[me], s1.at[j], r1.at[me], device))
        sends[-1].start()
    recv1[me] = send1[pair, pl.ds(pl.multiple_of(ROWS * slice_m, ROWS), ROWS)]
    rtotal1[me] = total1[pair]

    r = lax.broadcasted_iota(jnp.int32, (ROWS, DK), 0)
    lane = lax.broadcasted_iota(jnp.int32, (ROWS, DK), 1)
    is_key = lane == 16 * (r // 4) + 4 * slice_m + r % 4

    def column(row):
        return jnp.sum(jnp.where(is_key, row, 0.0), axis=1, keepdims=True)

    q = query_v[...].astype(F32)
    q = q * sigmoid(q)
    q_row = jnp.zeros((1, DK), F32)
    for n in range(2):
        for h in range(2):
            q_row += jnp.where(pair == 2 * n + h, q[n : n + 1, DK * h : DK * (h + 1)], 0.0)
    q_col = column(q_row)

    for j in range(1, PLANE):
        other, device = in_plane(j)
        remote(total1.at[0], rtotal1.at[other], st1.at[0], rt1.at[other], device).wait_recv()
        remote(rows_for(other), recv1.at[other], s1.at[0], r1.at[other], device).wait_recv()

    state = jnp.zeros((ROWS, DK), F32)
    total = jnp.zeros((1, DK), F32)
    for s in range(PLANE):
        row = rtotal1[s]
        state = column(jnp.exp(row)) * state + recv1[s].astype(F32)
        total = total + row
    send3[...] = state.astype(BF16)
    total3[...] = total

    for j in SENDS:
        other, device = in_line(j)
        sends.append(remote(total3, rtotal3.at[group], st3.at[j], rt3.at[group], device))
        sends[-1].start()
        sends.append(remote(send3, recv3.at[group], s3.at[j], r3.at[group], device))
        sends[-1].start()
    recv3[group] = send3[...]
    rtotal3[group] = total3[...]
    for j in SENDS[::-1]:
        other, device = in_line(j)
        remote(total3, rtotal3.at[other], st3.at[0], rt3.at[other], device).wait_recv()
        remote(send3, recv3.at[other], s3.at[0], r3.at[other], device).wait_recv()
    state = jnp.zeros((ROWS, DK), F32)
    for g in range(GROUPS):
        state = column(jnp.exp(rtotal3[g])) * state + recv3[g].astype(F32)

    part4[...] = jnp.sum(q_col * state, axis=0, keepdims=True)
    for j in range(1, PLANE):
        other, device = in_plane(j)
        sends.append(remote(part4, recv4.at[me], s4.at[j], r4.at[me], device))
        sends[-1].start()
    recv4[me] = part4[...]
    for i in range(4):
        row4[i] = jnp.sum(jnp.where(r == 4 * group + i, state, 0.0), axis=0, keepdims=True)

    def in_column(j):
        other = (pair + j) % 4
        return other, (sp - pair + other, tp)

    for j in range(1, 4):
        other, device = in_column(j)
        sends.append(remote(row4.at[other], rrow4.at[pair], sr4.at[j], rr4.at[pair], device))
        sends[-1].start()
    rrow4[pair] = row4[pair]

    g = gate_v[...].astype(F32)
    g = g * sigmoid(g)
    load_out.wait()
    for j in range(1, PLANE):
        other, device = in_plane(j)
        remote(part4, recv4.at[other], s4.at[0], r4.at[other], device).wait_recv()
    reads = []
    for p in range(4):
        n, h = p // 2, p % 2
        raw = recv4[p] + recv4[4 + p] + recv4[8 + p] + recv4[12 + p]
        scale = lax.rsqrt(jnp.mean(raw * raw, axis=-1, keepdims=True) + EPSILON)
        reads.append(raw * scale * gain_v[...] * g[n : n + 1, DK * h : DK * (h + 1)])
    row8 = lax.broadcasted_iota(jnp.int32, (8, DK), 0)
    heads = [jnp.where(row8 == 0, reads[h], jnp.where(row8 == 1, reads[2 + h], 0.0)) for h in range(2)]
    read = jnp.concatenate(heads, axis=1).astype(BF16)
    width = decode_out.shape[1]
    for t in range(N_TP):
        term = jnp.dot(read, wo_v[:, t * width : (t + 1) * width], preferred_element_type=F32)
        send5[t] = term[0:2].astype(BF16)

    for j in range(1, N_TP):
        other, device = in_tp(j)
        sends.append(remote(send5.at[other], recv5.at[tp], s5.at[j], r5.at[tp], device))
        sends[-1].start()
    recv5[tp] = send5[tp]
    for j in range(1, 4):
        other, device = in_column(j)
        remote(row4.at[0], rrow4.at[other], sr4.at[0], rr4.at[other], device).wait_recv()
    for p in range(4):
        state_out[p // 2, p % 2] = rrow4[p].astype(BF16)
    for j in range(1, N_TP):
        other, device = in_tp(j)
        remote(send5.at[0], recv5.at[other], s5.at[0], r5.at[other], device).wait_recv()
    out = recv5[0].astype(F32)
    for t in range(1, N_TP):
        out += recv5[t].astype(F32)
    decode_out[...] = out.astype(BF16)
    for copy in sends:
        copy.wait_send()


def on_device(tokens, w_forget, w_value, floor_logit, norm_gain, query_new, gate_new, w_out):
    flat = tokens.reshape(-1, tokens.shape[-1])
    any_spec = pl.BlockSpec(memory_space=pl.ANY)
    vmem_spec = pl.BlockSpec(memory_space=pltpu.VMEM)
    dma = pltpu.SemaphoreType.DMA
    return pl.pallas_call(
        kernel,
        name="final_states",
        out_shape=(
            jax.ShapeDtypeStruct((2, 2, 1, DK), BF16),
            jax.ShapeDtypeStruct((2, w_out.shape[1] // N_TP), BF16),
        ),
        in_specs=[any_spec] * 8,
        out_specs=(vmem_spec, vmem_spec),
        scratch_shapes=[
            pltpu.VMEM(flat.shape, BF16),
            pltpu.VMEM(w_forget.shape, BF16),
            pltpu.VMEM(w_value.shape, BF16),
            pltpu.VMEM(w_out.shape, BF16),
            pltpu.VMEM((1, 2 * DK), F32),
            pltpu.VMEM((1, DK), F32),
            pltpu.VMEM((2, 2 * DK), BF16),
            pltpu.VMEM((2, 2 * DK), BF16),
            pltpu.VMEM((4, DK, DK), BF16),
            pltpu.VMEM((4, 1, DK), F32),
            pltpu.VMEM((PLANE, ROWS, DK), BF16),
            pltpu.VMEM((PLANE, 1, DK), F32),
            pltpu.VMEM((ROWS, DK), BF16),
            pltpu.VMEM((1, DK), F32),
            pltpu.VMEM((GROUPS, ROWS, DK), BF16),
            pltpu.VMEM((GROUPS, 1, DK), F32),
            pltpu.VMEM((1, DK), F32),
            pltpu.VMEM((PLANE, 1, DK), F32),
            pltpu.VMEM((4, 1, DK), F32),
            pltpu.VMEM((4, 1, DK), F32),
            pltpu.VMEM((N_TP, 2, w_out.shape[1] // N_TP), BF16),
            pltpu.VMEM((N_TP, 2, w_out.shape[1] // N_TP), BF16),
            dma((3 * CHUNKS,)),
            dma((4,)),
            dma,
            dma((PLANE,)), dma((PLANE,)), dma((PLANE,)), dma((PLANE,)),
            dma((GROUPS,)), dma((GROUPS,)), dma((GROUPS,)), dma((GROUPS,)),
            dma((PLANE,)), dma((PLANE,)), dma((4,)), dma((4,)),
            dma((N_TP,)), dma((N_TP,)),
        ],
        compiler_params=pltpu.CompilerParams(collective_id=0, has_side_effects=True),
    )(flat, w_forget, w_value, floor_logit.reshape(1, -1), norm_gain.reshape(1, -1), query_new, gate_new, w_out)


def solution(mesh):
    return jax.shard_map(
        on_device,
        mesh=mesh,
        in_specs=(
            P(None, "sp", None),
            P(None, "tp"),
            P(None, "tp"),
            P("tp"),
            P(),
            P(None, "tp"),
            P(None, "tp"),
            P("tp", None),
        ),
        out_specs=(P(None, "tp", "sp", None), P(None, "tp")),
        check_vma=False,
    )
```

```python
import functools

import jax
import jax.numpy as jnp
from jax import lax
from jax.experimental import pallas as pl
from jax.experimental.pallas import tpu as pltpu
from jax.sharding import PartitionSpec as P

MESH = pl.DeviceIdType.MESH
F32 = jnp.float32
BF16 = jnp.bfloat16
EPSILON = 1e-06

DK = 128
SPAN = 64
NY = 4
NZ = 32
N_TP = 8
CHUNKS = 4
TURN = 17
ORDER = sorted(range(1, NZ), key=lambda z: 11 + 1.55 * z if z < TURN else 30 + 0.6 * (NZ - z))


def kernel(
    tok, w_forget, w_value, floor, gain, query, gate, w_out,
    state_out, decode_out,
    tok_v, wf_v, wv_v, wcols, floor_v, gain_v, query_v, gate_v,
    send1, total1, recv1, rtotal1,
    send3, total3, recv3, rtotal3,
    read4, recv4, final, block, row5, rrow5, decode,
    in_sem, small_sem, w_own, w_send, w_recv,
    s1, r1, st1, rt1, s3, r3, st3, rt3, s4, r4, sblock, rblock, s5, r5, sdec, rdec,
):
    sp, tp = lax.axis_index("sp"), lax.axis_index("tp")
    z, pair = sp // NY, sp % NY
    depth = tok.shape[1] // CHUNKS
    width = decode.shape[1]

    loads = []
    for c in range(CHUNKS):
        ks = pl.ds(c * depth, depth)
        loads.append([
            pltpu.make_async_copy(tok.at[:, ks], tok_v.at[:, ks], in_sem.at[3 * c]),
            pltpu.make_async_copy(w_forget.at[ks], wf_v.at[ks], in_sem.at[3 * c + 1]),
            pltpu.make_async_copy(w_value.at[ks], wv_v.at[ks], in_sem.at[3 * c + 2]),
        ])
    smalls = [
        pltpu.make_async_copy(src, dst, small_sem.at[i])
        for i, (src, dst) in enumerate(((floor, floor_v), (gain, gain_v), (query, query_v), (gate, gate_v)))
    ]
    for copy in loads[0]:
        copy.start()
    for copy in smalls:
        copy.start()
    for chunk in loads[1:]:
        for copy in chunk:
            copy.start()

    barrier = pltpu.get_barrier_semaphore()

    def signal(device):
        pl.semaphore_signal(barrier, inc=1, device_id=device, device_id_type=MESH)

    def in_column(j):
        other = (pair + j) % NY
        return other, (sp - pair + other, tp)

    mine = pair * N_TP + tp

    def in_root(j):
        other = (mine + j) % (NY * N_TP)
        return other, (other // N_TP, other % N_TP)

    def in_line(other):
        return (other * NY + pair, tp)

    for j in range(1, NY):
        signal(in_column(j)[1])

    @pl.when(z == 0)
    def _():
        for other in range(1, NZ):
            signal(in_line(other))
        for j in range(1, NY * N_TP):
            if j % N_TP:
                signal(in_root(j)[1])

    def remote(src, dst, send_sem, recv_sem, device):
        return pltpu.make_async_remote_copy(
            src_ref=src, dst_ref=dst, send_sem=send_sem, recv_sem=recv_sem, device_id=device, device_id_type=MESH
        )

    forget_acc = jnp.zeros((2 * SPAN, 2 * DK), F32)
    value_acc = jnp.zeros((2 * SPAN, 2 * DK), F32)
    for c in range(CHUNKS):
        for copy in loads[c]:
            copy.wait()
        ks = pl.ds(c * depth, depth)
        part = tok_v[:, ks]
        forget_acc += jnp.dot(part, wf_v[ks, :], preferred_element_type=F32)
        value_acc += jnp.dot(part, wv_v[ks, :], preferred_element_type=F32)
    for copy in smalls:
        copy.wait()
    forget_pre = forget_acc.astype(BF16).astype(F32)
    values_t = value_acc.astype(BF16).astype(F32).T.astype(BF16)

    def sigmoid(x):
        return 1.0 / (1.0 + jnp.exp(-x))

    key_gate = sigmoid(-floor_v[...]) * sigmoid(-forget_pre)
    log_keep = jnp.log1p(-key_gate)
    for n in range(2):
        total = jnp.sum(log_keep[SPAN * n : SPAN * (n + 1)], axis=0, keepdims=True)
        for h in range(2):
            total1[2 * n + h] = total[:, DK * h : DK * (h + 1)]

    pos = lax.broadcasted_iota(jnp.int32, (128, 128), 0)
    lane = lax.broadcasted_iota(jnp.int32, (128, 128), 1)
    after = jnp.where((lane > pos) & (lane // SPAN == pos // SPAN), 1.0, 0.0).astype(F32)
    decay = jnp.dot(after, log_keep, preferred_element_type=F32, precision=lax.Precision.HIGHEST)
    weighted = key_gate * jnp.exp(decay)
    first = pos < SPAN
    for h in range(2):
        w = weighted[:, DK * h : DK * (h + 1)]
        both = jnp.concatenate([jnp.where(first, w, 0.0), jnp.where(first, 0.0, w)], axis=1).astype(BF16)
        own = jnp.dot(values_t[DK * h : DK * (h + 1)], both, preferred_element_type=F32).astype(BF16)
        for n in range(2):
            send1[2 * n + h] = own[:, DK * n : DK * (n + 1)]

    pl.semaphore_wait(barrier, jnp.where(z == 0, NY * N_TP - 1, NY))
    column = []
    for j in range(1, NY):
        other, device = in_column(j)
        column.append(remote(total1.at[other], rtotal1.at[pair], st1.at[j], rt1.at[pair], device))
        column.append(remote(send1.at[other], recv1.at[pair], s1.at[j], r1.at[pair], device))
    for copy in column:
        copy.start()
    recv1[pair] = send1[pair]
    rtotal1[pair] = total1[pair]

    def w_columns(t):
        return w_out.at[:, pl.ds(pl.multiple_of(width * t, width), width)]

    w_local = pltpu.make_async_copy(w_columns(tp), wcols.at[tp], w_own)

    def w_copy(j):
        other = (tp + j) % N_TP
        return remote(w_columns(other), wcols.at[tp], w_send.at[j], w_recv.at[tp], (sp, other))

    @pl.when(z == 0)
    def _():
        for j in range(1, N_TP):
            w_copy(j).start()
        w_local.start()

    for j in range(1, NY):
        other, device = in_column(j)
        remote(total1.at[0], rtotal1.at[other], st1.at[0], rt1.at[other], device).wait_recv()
        remote(send1.at[0], recv1.at[other], s1.at[0], r1.at[other], device).wait_recv()
    state = recv1[0].astype(F32)
    total = rtotal1[0]
    for s in range(1, NY):
        row = rtotal1[s]
        state = jnp.exp(row) * state + recv1[s].astype(F32)
        total = total + row
    send3[...] = state.astype(BF16)
    total3[...] = total

    def pass_rows():
        r8 = lax.broadcasted_iota(jnp.int32, (8, DK), 0)
        rows = block[...]
        for i in range(NY):
            row5[i] = jnp.sum(jnp.where(r8 == NY * (z % 2) + i, rows, 0.0), axis=0, keepdims=True)
        for j in range(1, NY):
            other, device = in_column(j)
            remote(row5.at[other], rrow5.at[pair], s5.at[j], r5.at[pair], device).start()
        rrow5[pair] = row5[pair]

    def wait_rows():
        for j in range(1, NY):
            other, device = in_column(j)
            remote(row5.at[0], rrow5.at[other], s5.at[0], r5.at[other], device).wait_recv()

    def state_to_root(source):
        return (
            remote(total3, rtotal3.at[source], st3, rt3.at[source], in_line(0)),
            remote(send3, recv3.at[source], s3, r3.at[source], in_line(0)),
        )

    def block_to(other):
        rows = pl.ds(8 * (other // 2), 8)
        return remote(final.at[rows], block, sblock.at[other], rblock, in_line(other))

    def decode_to(other):
        return remote(decode, decode, sdec.at[other], rdec, in_line(other))

    @pl.when(z != 0)
    def _():
        for copy in state_to_root(z):
            copy.start()
        block_to(1).wait_recv()
        pass_rows()
        wait_rows()
        decode_to(1).wait_recv()
        for copy in state_to_root(z):
            copy.wait_send()

    @pl.when(z == 0)
    def _():
        def of_pair(x):
            row = jnp.zeros((1, DK), F32)
            for p in range(NY):
                n, h = p // 2, p % 2
                row += jnp.where(pair == p, x[n : n + 1, DK * h : DK * (h + 1)], 0.0)
            return row * sigmoid(row)

        q_row = of_pair(query_v[...].astype(F32))
        out_gate = gain_v[...] * of_pair(gate_v[...].astype(F32))
        lower = send3[...].astype(F32)
        upper = jnp.zeros((DK, DK), F32)
        upper_keep = jnp.ones((1, DK), F32)
        for i, source in enumerate(ORDER):
            if i == 20:
                pass
            for copy in state_to_root(source):
                copy.wait_recv()
            keep = jnp.exp(rtotal3[source])
            incoming = recv3[source].astype(F32)
            if source < TURN:
                lower = keep * lower + incoming
            else:
                upper = upper + upper_keep * incoming
                upper_keep = upper_keep * keep
        state_t = upper + upper_keep * lower

        raw = jnp.sum(q_row * state_t, axis=1, keepdims=True)
        scale = lax.rsqrt(jnp.mean(raw * raw, axis=0, keepdims=True) + EPSILON)
        raw_row = jnp.sum(jnp.where(pos == lane, raw, 0.0), axis=0, keepdims=True)
        read4[...] = raw_row * scale * out_gate
        for j in range(1, NY * N_TP):
            other, device = in_root(j)
            remote(read4, recv4.at[mine], s4.at[j], r4.at[mine], device).start()
        recv4[mine] = read4[...]

        rows = state_t.T
        final[...] = rows
        block[...] = rows[0:8]
        for other in range(1, NZ):
            block_to(other).start()
        pass_rows()
        for j in range(1, N_TP):
            other = (tp + j) % N_TP
            remote(w_columns(0), wcols.at[other], w_send.at[0], w_recv.at[other], (sp, other)).wait_recv()
        w_local.wait()

        for j in range(1, NY * N_TP):
            other, device = in_root(j)
            remote(read4, recv4.at[other], s4.at[0], r4.at[other], device).wait_recv()
        r8 = lax.broadcasted_iota(jnp.int32, (8, DK), 0)
        out = jnp.zeros((8, width), F32)
        for t in range(N_TP):
            heads = [
                jnp.where(r8 == 0, recv4[h * N_TP + t], jnp.where(r8 == 1, recv4[(2 + h) * N_TP + t], 0.0))
                for h in range(2)
            ]
            read = jnp.concatenate(heads, axis=1).astype(BF16)
            out += jnp.dot(read, wcols[t], preferred_element_type=F32).astype(BF16).astype(F32)
        decode[...] = out[0:2].astype(BF16)
        for other in range(1, NZ):
            decode_to(other).start()
        wait_rows()
        for j in range(1, N_TP):
            w_copy(j).wait_send()
        for j in range(1, NY * N_TP):
            remote(read4, recv4.at[mine], s4.at[j], r4.at[mine], in_root(j)[1]).wait_send()
        for other in range(1, NZ):
            block_to(other).wait_send()
        for other in range(1, NZ):
            decode_to(other).wait_send()

    for copy in column:
        copy.wait_send()
    for j in range(1, NY):
        remote(row5.at[0], rrow5.at[pair], s5.at[j], r5.at[pair], in_column(j)[1]).wait_send()
    for p in range(NY):
        n, h = p // 2, p % 2
        state_out[n, h : h + 1] = rrow5[p].astype(BF16)
    decode_out[...] = decode[...]


def on_device(tokens, w_forget, w_value, floor_logit, norm_gain, query_new, gate_new, w_out):
    flat = tokens.reshape(-1, tokens.shape[-1])
    width = w_out.shape[1] // N_TP
    any_spec = pl.BlockSpec(memory_space=pl.ANY)
    vmem_spec = pl.BlockSpec(memory_space=pltpu.VMEM)
    dma = pltpu.SemaphoreType.DMA
    state, decode = pl.pallas_call(
        kernel,
        name="final_states",
        out_shape=(pltpu.VMEM((2, 2, DK), BF16), pltpu.VMEM((2, width), BF16)),
        in_specs=[any_spec] * 8,
        out_specs=(vmem_spec, vmem_spec),
        scratch_shapes=[
            pltpu.VMEM(flat.shape, BF16),
            pltpu.VMEM(w_forget.shape, BF16),
            pltpu.VMEM(w_value.shape, BF16),
            pltpu.VMEM((N_TP, w_out.shape[0], width), BF16),
            pltpu.VMEM((1, 2 * DK), F32),
            pltpu.VMEM((1, DK), F32),
            pltpu.VMEM((2, 2 * DK), BF16),
            pltpu.VMEM((2, 2 * DK), BF16),
            pltpu.VMEM((NY, DK, DK), BF16),
            pltpu.VMEM((NY, 1, DK), F32),
            pltpu.VMEM((NY, DK, DK), BF16),
            pltpu.VMEM((NY, 1, DK), F32),
            pltpu.VMEM((DK, DK), BF16),
            pltpu.VMEM((1, DK), F32),
            pltpu.VMEM((NZ, DK, DK), BF16),
            pltpu.VMEM((NZ, 1, DK), F32),
            pltpu.VMEM((1, DK), F32),
            pltpu.VMEM((NY * N_TP, 1, DK), F32),
            pltpu.VMEM((DK, DK), F32),
            pltpu.VMEM((8, DK), F32),
            pltpu.VMEM((NY, 1, DK), F32),
            pltpu.VMEM((NY, 1, DK), F32),
            pltpu.VMEM((2, width), BF16),
            dma((3 * CHUNKS,)), dma((4,)), dma, dma((N_TP,)), dma((N_TP,)),
            dma((NY,)), dma((NY,)), dma((NY,)), dma((NY,)),
            dma, dma((NZ,)), dma, dma((NZ,)),
            dma((NY * N_TP,)), dma((NY * N_TP,)),
            dma((NZ,)), dma, dma((NY,)), dma((NY,)), dma((NZ,)), dma,
        ],
        compiler_params=pltpu.CompilerParams(collective_id=0, has_side_effects=True),
    )(flat, w_forget, w_value, floor_logit.reshape(1, -1), norm_gain.reshape(1, -1), query_new, gate_new, w_out)
    return state.reshape(2, 2, 1, DK), decode


def solution(mesh):
    return jax.shard_map(
        on_device,
        mesh=mesh,
        in_specs=(
            P(None, "sp", None),
            P(None, "tp"),
            P(None, "tp"),
            P("tp"),
            P(),
            P(None, "tp"),
            P(None, "tp"),
            P("tp", None),
        ),
        out_specs=(P(None, "tp", "sp", None), P(None, "tp")),
        check_vma=False,
    )
```
